32 devices in a mesh: grp: 2 (over y), ra: 4 (over z), cb: 2 (over x), dp: 2 (over core).
Axes of the slice: x: 2, y: 2, z: 4, core: 2. Of those that a mesh axis runs over, the one named last changes fastest.
Arguments:
- tokens: bfloat16 [256, 2048], P(('grp', 'dp'), 'ra'), parts along dimension 0, may hold values from -62 to 62
- gain_first: float32 [2048], P('ra'), may hold values from 0.1 to 1.9
- up_first: bfloat16 [2048, 8192], P('ra', 'cb'), may hold values from -0.125 to 0.125
- down_first: bfloat16 [8192, 2048], P('cb', 'ra'), may hold values from -0.0625 to 0.0625
- gain_second: float32 [2048], P('ra'), may hold values from 0.1 to 1.9
- up_second: bfloat16 [2048, 8192], P('ra', 'cb'), may hold values from -0.125 to 0.125
- down_second: bfloat16 [8192, 2048], P('cb', 'ra'), may hold values from -0.0625 to 0.0625
- gain_last: float32 [2048], P('ra'), may hold values from 0.1 to 1.9
Outputs:
- normed: bfloat16 [256, 2048], P(('grp', 'dp'), 'ra'), parts along dimension 0
The draws below stay inside these ranges and needn't reach their ends.
There are 2 independent parts, one for each index of `grp`. The reference program is written for one: setup_inputs(seed, part) draws one part's arguments, and reference() takes and returns one part's arrays. A program takes and returns all parts, laid end to end along the dimension named above; an argument that names none is the same for every part. Nothing has to cross between parts.
All inputs are finite; a program needn't handle non-finite values.
Results may differ from the reference program's by a relative error of at most 0.0095.
Values may be sent and summed in bfloat16 or wider, within the bound.
A program may use at most 64 MiB of HBM per device.

```python
import jax
import jax.numpy as jnp
from jax import lax

D = 2048
FF = 8192
TOKENS = 128


def draw_tokens(key, part):
    key_base = jax.random.fold_in(key, 11)
    key_cols = jax.random.fold_in(key, 12)
    key_rows = jax.random.fold_in(key, 13)
    position = jnp.arange(D, dtype=jnp.float32) / D
    columns = 10.0 ** (position - 0.5) * jnp.exp(jax.random.uniform(key_cols, (D,), jnp.float32, -0.7, 0.7))
    base = jnp.clip(jax.random.normal(key_base, (TOKENS, D), jnp.float32), -6.0, 6.0)
    rows = jnp.exp(jax.random.uniform(key_rows, (TOKENS, 1), jnp.float32, -1.15, 1.15))
    return jnp.clip(base * rows * columns, -62.0, 62.0).astype(jnp.bfloat16)


def steps_of(key, shape, shards, low, high):
    def one(axis_at, blocks):
        steps = jax.random.uniform(jax.random.fold_in(jax.random.fold_in(key, 6), axis_at), (blocks,), jnp.float32, low / len(shards), high / len(shards))
        return jnp.repeat(jnp.exp(steps), shape[axis_at] // blocks).reshape((-1,) + (1,) * (len(shape) - axis_at - 1))

    loudness = one(*shards[0])
    for cut in shards[1:]:
        loudness = loudness * one(*cut)
    return loudness


def normal_values(stream_key, dims, scale, bound, split=(), kind=jnp.bfloat16):
    result = scale * jax.random.normal(stream_key, dims, jnp.float32)
    if split:
        result = result * steps_of(stream_key, dims, split, -0.22, 0.18)
    return jnp.clip(result, -bound, bound).astype(kind)


def setup_inputs(seed: int = 0, part: int = 0) -> dict:
    arg_keys = jax.random.split(jax.random.key(seed), 9)
    part_keys = jax.random.split(jax.random.fold_in(arg_keys[8], part), 9)
    tokens = draw_tokens(jax.random.fold_in(jax.random.fold_in(arg_keys[8], part), 71), part)
    gain_first = jnp.clip(1.0 + 0.18 * jax.random.normal(arg_keys[1], (D,), jnp.float32), 0.1, 1.9)
    up_first = normal_values(arg_keys[2], (D, FF), D ** -0.5, 0.125, ((0, 4), (1, 2)))
    down_first = normal_values(arg_keys[3], (FF, D), FF ** -0.5, 0.0625, ((0, 2), (1, 4)))
    gain_second = jnp.clip(1.0 + 0.18 * jax.random.normal(arg_keys[4], (D,), jnp.float32), 0.1, 1.9)
    up_second = normal_values(arg_keys[5], (D, FF), D ** -0.5, 0.125, ((0, 4), (1, 2)))
    down_second = normal_values(arg_keys[6], (FF, D), FF ** -0.5, 0.0625, ((0, 2), (1, 4)))
    gain_last = jnp.clip(1.0 + 0.18 * jax.random.normal(arg_keys[7], (D,), jnp.float32), 0.1, 1.9)
    return dict(tokens=tokens, gain_first=gain_first, up_first=up_first, down_first=down_first, gain_second=gain_second, up_second=up_second, down_second=down_second, gain_last=gain_last)


EPS = 1e-06

def norm_inverse(h32):
    return lax.rsqrt(lax.optimization_barrier(jnp.mean(h32 * h32, axis=1, keepdims=True)) + EPS)

def mlp_branch(h32, gain, w_up, w_down):
    scaled = (h32 * gain).astype(jnp.bfloat16)
    pre = jnp.dot(scaled, w_up, preferred_element_type=jnp.float32) * norm_inverse(h32)
    hidden = jnp.square(jax.nn.relu(pre)).astype(jnp.bfloat16)
    return jnp.dot(hidden, w_down, preferred_element_type=jnp.float32)

def reference(tokens, gain_first, up_first, down_first, gain_second, up_second, down_second, gain_last):
    start32 = tokens.astype(jnp.float32)
    first = (0.5 * start32 + mlp_branch(start32, gain_first, up_first, down_first)).astype(jnp.bfloat16)
    first32 = first.astype(jnp.float32)
    second = (0.5 * first32 + mlp_branch(first32, gain_second, up_second, down_second)).astype(jnp.bfloat16)
    second32 = second.astype(jnp.float32)
    return (second32 * norm_inverse(second32) * gain_last).astype(jnp.bfloat16)
```

```python
import functools

import jax
import jax.numpy as jnp
from jax import lax
from jax.experimental import pallas as pl
from jax.experimental.pallas import tpu as pltpu
from jax.sharding import PartitionSpec as P

EPS = 1e-06
MESH = pl.DeviceIdType.MESH
F32, BF16 = jnp.float32, jnp.bfloat16

CHUNK = 1024
SPLITS = 4
PIECES = 2
LAG10 = 50
SLACK = 3


def kernel(
    n,
    ncb,
    width,
    tokens_ref,
    gain_first,
    up_first,
    down_first,
    gain_second,
    up_second,
    down_second,
    gain_last,
    out_ref,
    tokens_v,
    gain_v,
    out_v,
    up_v,
    down_v,
    h_v,
    scaled_v,
    own_v,
    acc_v,
    branch_v,
    inv_v,
    send_v,
    recv_v,
    sq_send,
    sq_recv,
    cb_send,
    cb_recv,
    in_sem,
    out_sem,
    up_sem,
    weight_sem,
    send_sem,
    recv_sem,
    sq_ssem,
    sq_rsem,
    cb_ssem,
    cb_rsem,
):
    k = lax.axis_index("ra")
    cb = lax.axis_index("cb")
    hidden = up_v.shape[2]
    splits, rows = h_v.shape[0], h_v.shape[1]
    chunk = own_v.shape[2]
    pieces = send_v.shape[2]
    piece = chunk // pieces
    chunks = hidden // chunk
    jobs = splits * chunks
    swap = ncb == 2 and splits >= 2
    early = jnp.where(2 * k < n, 0, 1)
    late = 1 - early
    early_hops = jnp.where(early == 0, k, n - 1 - k)
    has_early = early_hops > 0
    early_to = jnp.where(early == 0, k + 1, k - 1)
    late_to = jnp.where(early_hops > 0, jnp.where(late == 0, k + 1, k - 1), early_to)
    depth = jnp.maximum(((n - 1 - 2 * early_hops) * LAG10 + 9) // 10, 1)
    deepest = max(((n - 1) * LAG10 + 9) // 10, 1)
    gap = max(0, chunks + deepest + SLACK - jobs)
    if swap:
        gap = max(gap, deepest - (splits - 2) * chunks, deepest + SLACK - (splits - 1) * chunks)
    period = jobs + gap

    def up_copy(c):
        columns = pl.ds(c * chunk, chunk)
        return pltpu.make_async_copy(up_first.at[:, columns], up_v.at[0, :, columns], up_sem.at[c])

    def up_wait(c):
        columns = pl.ds(pl.multiple_of(c * chunk, chunk), chunk)
        pltpu.make_async_copy(
            up_first.at[:, columns], up_v.at[0, :, columns], up_sem.at[c]
        ).wait()

    up_next = pltpu.make_async_copy(up_second, up_v.at[1], weight_sem.at[2])

    def down_copy(layer):
        ref = (down_first, down_second)[layer]
        return pltpu.make_async_copy(ref, down_v.at[layer], weight_sem.at[layer])

    def split_of(level, slot):
        if not swap:
            return slot
        swapped = (lax.rem(cb + level, 2) == 0) & (slot >= splits - 2)
        return jnp.where(swapped, 2 * splits - 3 - slot, slot)

    inputs = [pltpu.make_async_copy(tokens_ref, tokens_v, in_sem.at[0])]
    for i, ref in enumerate((gain_first, gain_second, gain_last)):
        inputs.append(pltpu.make_async_copy(ref, gain_v.at[i], in_sem.at[1 + i]))
    for copy in inputs:
        copy.start()
    for c in range(chunks):
        up_copy(c).start()

    barrier = pltpu.get_barrier_semaphore()
    partners = [
        (i, j) for i in range(n) for j in range(ncb) if i + j > 0 and (swap or i * j == 0)
    ]
    for i, j in partners:
        pl.semaphore_signal(
            barrier,
            inc=1,
            device_id={"ra": lax.rem(k + i, n), "cb": lax.rem(cb + j, ncb)},
            device_id_type=MESH,
        )
    for copy in inputs:
        copy.wait()
    for t in range(splits):
        h32 = tokens_v[t * rows : (t + 1) * rows, :].astype(F32)
        h_v[t] = h32
        scaled_v[0, t] = (h32 * gain_v[0]).astype(BF16)

    def multiply_first(c):
        up_wait(c)
        columns = pl.ds(pl.multiple_of(c * chunk, chunk), chunk)
        every = jnp.concatenate([scaled_v[0, t] for t in range(splits)], axis=0)
        product = jnp.dot(every, up_v[0, :, columns], preferred_element_type=F32)
        for t in range(splits):
            own_v[t * chunks + c] = product[t * rows : (t + 1) * rows, :]

    multiply_first(0)
    pl.semaphore_wait(barrier, len(partners))
    down_copy(0).start()
    up_next.start()
    down_copy(1).start()

    def chain(direction, job, p, to):
        return pltpu.make_async_remote_copy(
            src_ref=send_v.at[direction, job, p],
            dst_ref=recv_v.at[direction, job, p],
            send_sem=send_sem.at[direction],
            recv_sem=recv_sem.at[direction, lax.rem(job, jobs), p],
            device_id={"ra": to},
            device_id_type=MESH,
        )

    def sq_copy(level, t, to, to_cb):
        return pltpu.make_async_remote_copy(
            src_ref=sq_send.at[level, t],
            dst_ref=sq_recv.at[level, t, k],
            send_sem=sq_ssem,
            recv_sem=sq_rsem.at[level, t],
            device_id={"ra": to, "cb": to_cb},
            device_id_type=MESH,
        )

    def cb_copy(layer, t, to):
        return pltpu.make_async_remote_copy(
            src_ref=cb_send.at[layer, t],
            dst_ref=cb_recv.at[layer, t, cb],
            send_sem=cb_ssem,
            recv_sem=cb_rsem.at[layer, t],
            device_id={"cb": to},
            device_id_type=MESH,
        )

    def of_all(ref, ssem, rsem, axis, to):
        return pltpu.make_async_remote_copy(
            src_ref=ref,
            dst_ref=ref,
            send_sem=ssem,
            recv_sem=rsem,
            device_id={axis: to},
            device_id_type=MESH,
        )

    diagonal = lax.broadcasted_iota(jnp.int32, (rows, 128), 0) == lax.broadcasted_iota(
        jnp.int32, (rows, 128), 1
    )

    def send_squares(level, t, h32, across=False):
        total = jnp.sum(h32 * h32, axis=1, keepdims=True)
        line = jnp.sum(jnp.where(diagonal, total, 0.0), axis=0, keepdims=True)
        sq_send[level, t] = line
        sq_recv[level, t, k] = line
        for off in range(1, n):
            sq_copy(level, t, lax.rem(k + off, n), cb).start()
        if across:
            for off in range(n):
                sq_copy(level, t, lax.rem(k + off, n), lax.rem(cb + 1, ncb)).start()

    def wait_squares(level, t, count):
        peers = sq_recv.at[level, t, pl.ds(0, count)]
        of_all(peers, sq_ssem, sq_rsem.at[level, t], "ra", lax.rem(k + 1, n)).wait_recv()

    def inverse_of(level, t):
        total = sq_recv[level, t, 0]
        for source in range(1, n):
            total = total + sq_recv[level, t, source]
        line = lax.rsqrt(total * (1.0 / width) + EPS)
        column = jnp.sum(jnp.where(diagonal, line, 0.0), axis=1, keepdims=True)
        return jnp.broadcast_to(column, (rows, 128))

    def gather_branch(layer, t):
        peers = cb_recv.at[layer, t, pl.ds(0, ncb - 1)]
        of_all(peers, cb_ssem, cb_rsem.at[layer, t], "cb", lax.rem(cb + 1, ncb)).wait_recv()
        total = cb_recv[layer, t, 0].astype(F32)
        for source in range(1, ncb):
            total = total + cb_recv[layer, t, source].astype(F32)
        return (0.5 * h_v[t] + total).astype(BF16).astype(F32)

    def multiply_up(t, c):
        columns = pl.ds(pl.multiple_of(c * chunk, chunk), chunk)
        own_v[(splits + t) * chunks + c] = jnp.dot(
            scaled_v[1, t], up_v[1, :, columns], preferred_element_type=F32
        )

    def multiply_down(level, job, c):
        total = None
        for p in range(pieces):
            at = slice(p * piece, (p + 1) * piece)
            pre = (recv_v[late, job, p].astype(F32) + acc_v[job, :, at]) * inv_v[:, 0:1]
            act = jnp.square(jnp.maximum(pre, 0.0)).astype(BF16)
            rows_at = pl.ds(pl.multiple_of(c * chunk + p * piece, piece), piece)
            part = jnp.dot(act, down_v[level, rows_at, :], preferred_element_type=F32)
            total = part if total is None else total + part
        branch_v[...] = jnp.where(c == 0, 0.0, branch_v[...]) + total

    branch_v[...] = jnp.zeros_like(branch_v)

    def place(s):
        level = jnp.where(s < period, 0, jnp.where(s < 2 * period, 1, 2))
        at = s - level * period
        live = at < jobs
        slot = jnp.where(live, at // chunks, 0)
        return level, at, live, slot, at % chunks

    finals = [j for j in range(splits - 2 if swap else splits)]
    steps = 2 * jobs + gap + deepest
    inside = [j for j in finals if 2 * period + j * chunks < steps]

    def step(s, _):
        s2 = s - depth
        level2 = jnp.where(s2 < period, 0, 1)
        at2 = s2 - level2 * period
        live2 = (s2 >= 0) & (at2 < jobs)
        at2 = jnp.where(live2, at2, 0)
        t2 = split_of(level2, at2 // chunks)
        c2 = at2 % chunks
        job2 = level2 * jobs + at2

        level, at, live, slot, c = place(s)
        t = split_of(level, slot)
        job = level * jobs + at
        own_at = (level * splits + t) * chunks + c
        sending = live & (level < 2)

        own_at2 = (level2 * splits + t2) * chunks + c2
        for p in range(pieces):
            part = slice(p * piece, (p + 1) * piece)

            @pl.when(live2)
            def _():
                chain(late, job2, p, late_to).wait_recv()

                @pl.when(has_early)
                def _():
                    total = recv_v[late, job2, p].astype(F32) + own_v[own_at2, :, part]
                    send_v[late, job2, p] = total.astype(BF16)
                    chain(late, job2, p, late_to).start()

            @pl.when(sending)
            def _():
                own = own_v[own_at, :, part]

                @pl.when(has_early)
                def _():
                    chain(early, job, p, early_to).wait_recv()
                    total = recv_v[early, job, p].astype(F32) + own
                    send_v[early, job, p] = total.astype(BF16)
                    acc_v[job, :, part] = total

                @pl.when(jnp.logical_not(has_early))
                def _():
                    send_v[early, job, p] = own.astype(BF16)
                    acc_v[job, :, part] = own

                chain(early, job, p, early_to).start()

        @pl.when(s == 0)
        def _():
            for i in range(splits):
                send_squares(0, i, h_v[i])

        @pl.when(sending & (level == 1) & (c == 0))
        def _():
            send_squares(1, t, h_v[t])

        @pl.when(live2 & (c2 == 0))
        def _():
            wait_squares(level2, t2, n - 1)
            inv_v[...] = inverse_of(level2, t2)

        for layer in range(2):

            @pl.when(live2 & (job2 == layer * jobs))
            def _():
                down_copy(layer).wait()

        level3, at3, live3, slot3, c3 = place(s + 1)
        t3 = split_of(level3, slot3)
        ahead = live3 & (level3 == 1)
        both = live2 & ahead & (c3 > 0)

        @pl.when(both)
        def _():
            multiply_up(t3, c3)
            multiply_down(level2, job2, c2)

        @pl.when(live2 & jnp.logical_not(both))
        def _():
            multiply_down(level2, job2, c2)

        @pl.when(live2 & (c2 == chunks - 1))
        def _():
            value = branch_v[...].astype(BF16)
            cb_send[level2, t2] = value
            cb_recv[level2, t2, cb] = value
            for off in range(1, ncb):
                cb_copy(level2, t2, lax.rem(cb + off, ncb)).start()

        @pl.when(ahead & (c3 == 0))
        def _():
            h32 = gather_branch(0, t3)
            h_v[t3] = h32
            scaled_v[1, t3] = (h32 * gain_v[1]).astype(BF16)

            @pl.when(at3 == 0)
            def _():
                up_next.wait()

        @pl.when(ahead & jnp.logical_not(both))
        def _():
            multiply_up(t3, c3)

        @pl.when(live3 & (level3 == 0) & (at3 < chunks))
        def _():
            multiply_first(c3)

        for j in inside:

            @pl.when(s == 2 * period + j * chunks)
            def _():
                h32 = gather_branch(1, j)
                h_v[j] = h32
                send_squares(2, j, h32)

        return 0

    lax.fori_loop(0, steps, step, 0)

    def out_copy(t):
        at = pl.ds(pl.multiple_of(t * rows, rows), rows)
        return pltpu.make_async_copy(out_v.at[at, :], out_ref.at[at, :], out_sem)

    def finish(t):
        inv = inverse_of(2, t)[:, 0:1]
        at = pl.ds(pl.multiple_of(t * rows, rows), rows)
        out_v[at, :] = (h_v[t] * inv * gain_v[2]).astype(BF16)
        out_copy(t).start()

    if swap:
        mine = split_of(1, splits - 1)
        other = split_of(1, splits - 2)
        h32 = gather_branch(1, mine)
        h_v[mine] = h32
        send_squares(2, mine, h32, across=True)
    for j in finals:
        if j not in inside:
            h32 = gather_branch(1, j)
            h_v[j] = h32
            send_squares(2, j, h32)
    for j in finals:
        wait_squares(2, j, n - 1)
        finish(j)
    if swap:
        h_v[other] = gather_branch(1, other)
        wait_squares(2, other, n)
        finish(other)
        wait_squares(2, mine, n - 1)
        finish(mine)

    of_all(send_v.at[early], send_sem.at[early], recv_sem.at[early, 0, 0], "ra", early_to).wait_send()

    @pl.when(has_early)
    def _():
        of_all(send_v.at[late], send_sem.at[late], recv_sem.at[late, 0, 0], "ra", late_to).wait_send()

    peers = sq_recv.at[:, :, pl.ds(0, n - 1)]
    of_all(peers, sq_ssem, sq_rsem.at[0, 0], "ra", lax.rem(k + 1, n)).wait_send()
    if swap:
        one = sq_recv.at[0, 0, pl.ds(0, 1)]
        of_all(one, sq_ssem, sq_rsem.at[0, 0], "ra", lax.rem(k + 1, n)).wait_send()
    peers = cb_recv.at[:, :, pl.ds(0, ncb - 1)]
    of_all(peers, cb_ssem, cb_rsem.at[0, 0], "cb", lax.rem(cb + 1, ncb)).wait_send()
    pltpu.make_async_copy(out_v, out_ref, out_sem).wait()


def local(n, ncb, *args):
    tokens, gain_first, up_first, down_first, gain_second, up_second, down_second, gain_last = args
    rows, cols = tokens.shape
    hidden = up_first.shape[1]
    chunk = min(CHUNK, hidden)
    chunks = hidden // chunk
    splits = SPLITS if rows % (16 * SPLITS) == 0 else 1
    part = rows // splits
    jobs = splits * chunks
    piece = chunk // PIECES
    hbm = pl.BlockSpec(memory_space=pl.ANY)
    dma = pltpu.SemaphoreType.DMA
    return pl.pallas_call(
        functools.partial(kernel, n, ncb, cols * n),
        out_shape=jax.ShapeDtypeStruct((rows, cols), BF16),
        in_specs=[hbm] * 8,
        out_specs=hbm,
        scratch_shapes=[
            pltpu.VMEM((rows, cols), BF16),
            pltpu.VMEM((3, 1, cols), F32),
            pltpu.VMEM((rows, cols), BF16),
            pltpu.VMEM((2, cols, hidden), BF16),
            pltpu.VMEM((2, hidden, cols), BF16),
            pltpu.VMEM((splits, part, cols), F32),
            pltpu.VMEM((2, splits, part, cols), BF16),
            pltpu.VMEM((2 * jobs, part, chunk), F32),
            pltpu.VMEM((2 * jobs, part, chunk), F32),
            pltpu.VMEM((part, cols), F32),
            pltpu.VMEM((part, 128), F32),
            pltpu.VMEM((2, 2 * jobs, PIECES, part, piece), BF16),
            pltpu.VMEM((2, 2 * jobs, PIECES, part, piece), BF16),
            pltpu.VMEM((3, splits, 1, 128), F32),
            pltpu.VMEM((3, splits, n, 1, 128), F32),
            pltpu.VMEM((2, splits, part, cols), BF16),
            pltpu.VMEM((2, splits, ncb, part, cols), BF16),
            dma((4,)),
            dma,
            dma((chunks,)),
            dma((3,)),
            dma((2,)),
            dma((2, jobs, PIECES)),
            dma,
            dma((3, splits)),
            dma,
            dma((2, splits)),
        ],
        compiler_params=pltpu.CompilerParams(
            collective_id=0, has_side_effects=True, vmem_limit_bytes=60 * 1024 * 1024
        ),
    )(
        tokens,
        gain_first.reshape(1, cols),
        up_first,
        down_first,
        gain_second.reshape(1, cols),
        up_second,
        down_second,
        gain_last.reshape(1, cols),
    )


def solution(mesh):
    return jax.shard_map(
        functools.partial(local, mesh.shape["ra"], mesh.shape["cb"]),
        mesh=mesh,
        in_specs=(
            P(("grp", "dp"), "ra"),
            P("ra"),
            P("ra", "cb"),
            P("cb", "ra"),
            P("ra"),
            P("ra", "cb"),
            P("cb", "ra"),
            P("ra"),
        ),
        out_specs=P(("grp", "dp"), "ra"),
        check_vma=False,
    )
```

```python
import functools

import jax
import jax.numpy as jnp
from jax import lax
from jax.experimental import pallas as pl
from jax.experimental.pallas import tpu as pltpu
from jax.sharding import PartitionSpec as P

EPS = 1e-06
MESH = pl.DeviceIdType.MESH
F32, BF16 = jnp.float32, jnp.bfloat16

CHUNK = 1024
SPLITS = 4
PIECES = 2
LAG10 = (45, 40)
SLACK = (3, 3)
LIMIT = 55100


def kernel(
    n,
    ncb,
    moved,
    width,
    tokens_ref,
    gains,
    up_first,
    down_first,
    up_second,
    down_second,
    out_ref,
    tokens_v,
    extra_v,
    done_v,
    back_v,
    up_v,
    down_v,
    h_v,
    entry_v,
    scaled_v,
    own_v,
    acc_v,
    branch_v,
    inv_v,
    send_v,
    recv_v,
    sq_send,
    sq_recv,
    cb_send,
    cb_recv,
    in_sem,
    pass_sem,
    up_sem,
    weight_sem,
    send_sem,
    recv_sem,
    sq_ssem,
    sq_rsem,
    cb_ssem,
    cb_rsem,
):
    k = lax.axis_index("ra")
    second = lax.axis_index("dp") > 0
    other_core = 1 - lax.axis_index("dp")
    cb = lax.axis_index("cb")
    hidden = up_v.shape[2]
    most, rows = h_v.shape[0], h_v.shape[1]
    chunk = own_v.shape[2]
    pieces = send_v.shape[2]
    piece = chunk // pieces
    chunks = hidden // chunk
    most_jobs = most * chunks
    swap = ncb == 2 and most - 2 * moved >= 2
    splits = jnp.where(second, most, most - 2 * moved)
    jobs = splits * chunks
    early = jnp.where(2 * k < n, 0, 1)
    late = 1 - early
    early_hops = jnp.where(early == 0, k, n - 1 - k)
    has_early = early_hops > 0
    early_to = jnp.where(early == 0, k + 1, k - 1)
    late_to = jnp.where(early_hops > 0, jnp.where(late == 0, k + 1, k - 1), early_to)
    lags = jnp.where(second, LAG10[1], LAG10[0])
    slack = jnp.where(second, SLACK[1], SLACK[0])
    depth = jnp.maximum(((n - 1 - 2 * early_hops) * lags + 9) // 10, 1)
    deepest = jnp.maximum(((n - 1) * lags + 9) // 10, 1)
    gap = jnp.maximum(chunks + deepest + slack - jobs, 0)
    if swap:
        gap = jnp.maximum(gap, deepest - (splits - 2) * chunks)
        gap = jnp.maximum(gap, deepest + slack - (splits - 1) * chunks)
    period = jobs + gap

    def up_copy(c):
        columns = pl.ds(c * chunk, chunk)
        return pltpu.make_async_copy(up_first.at[:, columns], up_v.at[0, :, columns], up_sem.at[c])

    def up_wait(c):
        columns = pl.ds(pl.multiple_of(c * chunk, chunk), chunk)
        pltpu.make_async_copy(
            up_first.at[:, columns], up_v.at[0, :, columns], up_sem.at[c]
        ).wait()

    up_next = pltpu.make_async_copy(up_second, up_v.at[1], weight_sem.at[2])

    def down_copy(layer):
        ref = (down_first, down_second)[layer]
        return pltpu.make_async_copy(ref, down_v.at[layer], weight_sem.at[layer])

    def split_of(level, slot):
        if not swap:
            return slot
        swapped = (lax.rem(cb + level, 2) == 0) & (slot >= splits - 2)
        return jnp.where(swapped, 2 * splits - 3 - slot, slot)

    tokens_in = pltpu.make_async_copy(tokens_ref, tokens_v, in_sem)
    tokens_in.start()
    up_copy(0).start()

    barrier = pltpu.get_barrier_semaphore()
    partners = [
        (i, j) for i in range(n) for j in range(ncb) if i + j > 0 and (swap or i * j == 0)
    ]
    for i, j in partners:
        pl.semaphore_signal(
            barrier,
            inc=1,
            device_id={"ra": lax.rem(k + i, n), "cb": lax.rem(cb + j, ncb)},
            device_id_type=MESH,
        )
    if moved:
        pl.semaphore_signal(
            barrier, inc=1, device_id={"dp": other_core}, device_id_type=MESH
        )

    def to_core(src, dst, i):
        return pltpu.make_async_remote_copy(
            src_ref=src,
            dst_ref=dst,
            send_sem=pass_sem.at[2 * i],
            recv_sem=pass_sem.at[2 * i + 1],
            device_id={"dp": other_core},
            device_id_type=MESH,
        )

    last = most - 1 - moved
    lent = to_core(tokens_v.at[pl.ds(last * rows, rows), :], extra_v, 0)
    given = to_core(done_v, back_v, 1)

    def tile_of(i):
        return i + jnp.where(second, moved, 0) if i > 1 else i

    tokens_in.wait()
    for c in range(1, chunks):
        up_copy(c).start()
    def multiply_first(c):
        up_wait(c)
        columns = pl.ds(pl.multiple_of(c * chunk, chunk), chunk)
        product = jnp.dot(entry_v[...], up_v[0, :, columns], preferred_element_type=F32)
        for i in range(most - moved):
            own_v[tile_of(i) * chunks + c] = product[i * rows : (i + 1) * rows, :]

    def multiply_extra():
        for c in range(chunks):
            columns = pl.ds(c * chunk, chunk)
            own_v[2 * chunks + c] = jnp.dot(
                scaled_v[0], up_v[0, :, columns], preferred_element_type=F32
            )

    ready = has_early
    for i in range(most - moved):
        tile = tokens_v[i * rows : (i + 1) * rows, :].astype(F32)
        h_v[tile_of(i)] = tile
        entry_v[i * rows : (i + 1) * rows, :] = (tile * gains[0:1, :]).astype(BF16)
    multiply_first(0)

    @pl.when(ready)
    def _():
        for c in range(1, chunks):
            multiply_first(c)

    pl.semaphore_wait(barrier, len(partners) + moved)
    if moved:

        @pl.when(jnp.logical_not(second))
        def _():
            lent.start()

    down_copy(0).start()
    up_next.start()
    down_copy(1).start()

    def chain(direction, job, p, to):
        return pltpu.make_async_remote_copy(
            src_ref=send_v.at[direction, job, p],
            dst_ref=recv_v.at[direction, job, p],
            send_sem=send_sem.at[direction],
            recv_sem=recv_sem.at[direction, lax.rem(job, most_jobs), p],
            device_id={"ra": to},
            device_id_type=MESH,
        )

    def sq_copy(level, t, to, to_cb):
        return pltpu.make_async_remote_copy(
            src_ref=sq_send.at[level, t],
            dst_ref=sq_recv.at[level, t, k],
            send_sem=sq_ssem,
            recv_sem=sq_rsem.at[level, t],
            device_id={"ra": to, "cb": to_cb},
            device_id_type=MESH,
        )

    def cb_copy(layer, t, to):
        return pltpu.make_async_remote_copy(
            src_ref=cb_send.at[layer, t],
            dst_ref=cb_recv.at[layer, t, cb],
            send_sem=cb_ssem,
            recv_sem=cb_rsem.at[layer, t],
            device_id={"cb": to},
            device_id_type=MESH,
        )

    def of_all(ref, ssem, rsem, axis, to):
        return pltpu.make_async_remote_copy(
            src_ref=ref,
            dst_ref=ref,
            send_sem=ssem,
            recv_sem=rsem,
            device_id={axis: to},
            device_id_type=MESH,
        )

    diagonal = lax.broadcasted_iota(jnp.int32, (rows, 128), 0) == lax.broadcasted_iota(
        jnp.int32, (rows, 128), 1
    )

    def send_squares(level, t, h32, across=False):
        total = jnp.sum(h32 * h32, axis=1, keepdims=True)
        line = jnp.sum(jnp.where(diagonal, total, 0.0), axis=0, keepdims=True)
        sq_send[level, t] = line
        sq_recv[level, t, k] = line
        for off in range(1, n):
            sq_copy(level, t, lax.rem(k + off, n), cb).start()
        if across:
            for off in range(n):
                sq_copy(level, t, lax.rem(k + off, n), lax.rem(cb + 1, ncb)).start()

    def wait_squares(level, t, count):
        peers = sq_recv.at[level, t, pl.ds(0, count)]
        of_all(peers, sq_ssem, sq_rsem.at[level, t], "ra", lax.rem(k + 1, n)).wait_recv()

    def inverse_of(level, t):
        total = sq_recv[level, t, 0]
        for source in range(1, n):
            total = total + sq_recv[level, t, source]
        line = lax.rsqrt(total * (1.0 / width) + EPS)
        column = jnp.sum(jnp.where(diagonal, line, 0.0), axis=1, keepdims=True)
        return jnp.broadcast_to(column, (rows, 128))

    def gather_branch(layer, t):
        peers = cb_recv.at[layer, t, pl.ds(0, ncb - 1)]
        of_all(peers, cb_ssem, cb_rsem.at[layer, t], "cb", lax.rem(cb + 1, ncb)).wait_recv()
        total = cb_recv[layer, t, 0].astype(F32)
        for source in range(1, ncb):
            total = total + cb_recv[layer, t, source].astype(F32)
        return (0.5 * h_v[t] + total).astype(BF16).astype(F32)

    def multiply_up(t, c):
        columns = pl.ds(pl.multiple_of(c * chunk, chunk), chunk)
        own_v[(most + t) * chunks + c] = jnp.dot(
            scaled_v[1 + t], up_v[1, :, columns], preferred_element_type=F32
        )

    def multiply_down(level, job, c):
        total = None
        for p in range(pieces):
            at = slice(p * piece, (p + 1) * piece)
            pre = (recv_v[late, job, p].astype(F32) + acc_v[job, :, at]) * inv_v[:, 0:1]
            act = jnp.square(jnp.maximum(pre, 0.0)).astype(BF16)
            rows_at = pl.ds(pl.multiple_of(c * chunk + p * piece, piece), piece)
            part = jnp.dot(act, down_v[level, rows_at, :], preferred_element_type=F32)
            total = part if total is None else total + part
        branch_v[...] = jnp.where(c == 0, 0.0, branch_v[...]) + total

    branch_v[...] = jnp.zeros_like(branch_v)

    def place(s):
        level = jnp.where(s < period, 0, jnp.where(s < 2 * period, 1, 2))
        at = s - level * period
        live = at < jobs
        slot = jnp.where(live, at // chunks, 0)
        return level, at, live, slot, at % chunks

    steps = 2 * jobs + gap + deepest
    plain = splits - 2 if swap else splits

    def close(j):
        h32 = gather_branch(1, j)
        h_v[j] = h32
        send_squares(2, j, h32)

    def step(s, _):
        s2 = s - depth
        level2 = jnp.where(s2 < period, 0, 1)
        at2 = s2 - level2 * period
        live2 = (s2 >= 0) & (at2 < jobs)
        at2 = jnp.where(live2, at2, 0)
        t2 = split_of(level2, at2 // chunks)
        c2 = at2 % chunks
        job2 = level2 * most_jobs + at2

        level, at, live, slot, c = place(s)
        t = split_of(level, slot)
        job = level * most_jobs + at
        own_at = (level * most + t) * chunks + c
        sending = live & (level < 2)

        own_at2 = (level2 * most + t2) * chunks + c2
        for p in range(pieces):
            part = slice(p * piece, (p + 1) * piece)

            @pl.when(live2)
            def _():
                chain(late, job2, p, late_to).wait_recv()

                @pl.when(has_early)
                def _():
                    total = recv_v[late, job2, p].astype(F32) + own_v[own_at2, :, part]
                    send_v[late, job2, p] = total.astype(BF16)
                    chain(late, job2, p, late_to).start()

            @pl.when(sending)
            def _():
                own = own_v[own_at, :, part]

                @pl.when(has_early)
                def _():
                    chain(early, job, p, early_to).wait_recv()
                    total = recv_v[early, job, p].astype(F32) + own
                    send_v[early, job, p] = total.astype(BF16)
                    acc_v[job, :, part] = total

                @pl.when(jnp.logical_not(has_early))
                def _():
                    send_v[early, job, p] = own.astype(BF16)
                    acc_v[job, :, part] = own

                chain(early, job, p, early_to).start()

        @pl.when(s == 0)
        def _():
            for i in range(most):

                @pl.when((i < splits) & jnp.logical_not(second & (i == 2 * moved) & (moved > 0)))
                def _():
                    send_squares(0, i, h_v[i])

        if moved:

            @pl.when(second & (s == chunks - 1))
            def _():
                lent.wait_recv()
                h32 = extra_v[...].astype(F32)
                h_v[2] = h32
                scaled_v[0] = (h32 * gains[0:1, :]).astype(BF16)
                multiply_extra()
                send_squares(0, 2, h32)

        @pl.when(sending & (level == 1) & (c == 0))
        def _():
            send_squares(1, t, h_v[t])

        @pl.when(live2 & (c2 == 0))
        def _():
            wait_squares(level2, t2, n - 1)
            inv_v[...] = inverse_of(level2, t2)

        for layer in range(2):

            @pl.when(live2 & (job2 == layer * most_jobs))
            def _():
                down_copy(layer).wait()

        level3, at3, live3, slot3, c3 = place(s + 1)
        t3 = split_of(level3, slot3)
        ahead = live3 & (level3 == 1)
        both = live2 & ahead & (c3 > 0)

        @pl.when(both)
        def _():
            multiply_up(t3, c3)
            multiply_down(level2, job2, c2)

        @pl.when(live2 & jnp.logical_not(both))
        def _():
            multiply_down(level2, job2, c2)

        @pl.when(live2 & (c2 == chunks - 1))
        def _():
            value = branch_v[...].astype(BF16)
            cb_send[level2, t2] = value
            cb_recv[level2, t2, cb] = value
            for off in range(1, ncb):
                cb_copy(level2, t2, lax.rem(cb + off, ncb)).start()

        @pl.when(ahead & (c3 == 0))
        def _():
            h32 = gather_branch(0, t3)
            h_v[t3] = h32
            scaled_v[1 + t3] = (h32 * gains[1:1 + 1, :]).astype(BF16)

            @pl.when(at3 == 0)
            def _():
                up_next.wait()

        @pl.when(ahead & jnp.logical_not(both))
        def _():
            multiply_up(t3, c3)

        @pl.when(live3 & (level3 == 0) & (at3 < chunks) & jnp.logical_not(ready))
        def _():
            multiply_first(c3)

        for j in range(most):

            @pl.when((j < plain) & (s == 2 * period + j * chunks))
            def _():
                close(j)

        return 0

    lax.fori_loop(0, steps, step, 0)

    def normed(t):
        inv = inverse_of(2, t)[:, 0:1]
        return (h_v[t] * inv * gains[2:3, :]).astype(BF16)

    def finish(t):
        row = t - jnp.where(second & (t > 2), moved, 0)
        out_ref[pl.ds(pl.multiple_of(row * rows, rows), rows), :] = normed(t)

    if swap:
        mine = split_of(1, splits - 1)
        other = split_of(1, splits - 2)
        h32 = gather_branch(1, mine)
        h_v[mine] = h32
        send_squares(2, mine, h32, across=True)
    for j in range(most):

        @pl.when((j < plain) & (2 * period + j * chunks >= steps))
        def _():
            close(j)

    order = [2, 0, 1] + list(range(3, most)) if moved else list(range(most))
    for j in order:

        @pl.when(j < plain)
        def _():
            wait_squares(2, j, n - 1)
            if moved and j == 2:

                @pl.when(second)
                def _():
                    done_v[...] = normed(2)
                    given.start()

                @pl.when(jnp.logical_not(second))
                def _():
                    finish(2)

            else:
                finish(j)

    if swap:
        h_v[other] = gather_branch(1, other)
        wait_squares(2, other, n)
        finish(other)
        wait_squares(2, mine, n - 1)
        finish(mine)

    def wait_sends(count):
        sent = 2 * count * chunks
        of_all(
            send_v.at[early, pl.ds(0, sent)],
            send_sem.at[early],
            recv_sem.at[early, 0, 0],
            "ra",
            early_to,
        ).wait_send()

        @pl.when(has_early)
        def _():
            of_all(
                send_v.at[late, pl.ds(0, sent)],
                send_sem.at[late],
                recv_sem.at[late, 0, 0],
                "ra",
                late_to,
            ).wait_send()

        peers = sq_recv.at[:, pl.ds(0, count), pl.ds(0, n - 1)]
        of_all(peers, sq_ssem, sq_rsem.at[0, 0], "ra", lax.rem(k + 1, n)).wait_send()
        if swap:
            one = sq_recv.at[0, 0, pl.ds(0, 1)]
            of_all(one, sq_ssem, sq_rsem.at[0, 0], "ra", lax.rem(k + 1, n)).wait_send()
        peers = cb_recv.at[:, pl.ds(0, count), pl.ds(0, ncb - 1)]
        of_all(peers, cb_ssem, cb_rsem.at[0, 0], "cb", lax.rem(cb + 1, ncb)).wait_send()

    if moved:

        @pl.when(second)
        def _():
            wait_sends(most)
            given.wait_send()

        @pl.when(jnp.logical_not(second))
        def _():
            wait_sends(most - 2)
            lent.wait_send()
            given.wait_recv()
            out_ref[last * rows : (last + 1) * rows, :] = back_v[...]

    else:
        wait_sends(most)


def local(n, ncb, ndp, *args):
    tokens, gain_first, up_first, down_first, gain_second, up_second, down_second, gain_last = args
    rows, cols = tokens.shape
    hidden = up_first.shape[1]
    chunk = min(CHUNK, hidden)
    chunks = hidden // chunk
    splits = SPLITS if rows % (16 * SPLITS) == 0 else 1
    part = rows // splits
    moved = int(ndp == 2 and splits >= 4)
    most = splits + moved
    jobs = most * chunks
    piece = chunk // PIECES
    hbm = pl.BlockSpec(memory_space=pl.ANY)
    vm = pl.BlockSpec(memory_space=pltpu.VMEM)
    dma = pltpu.SemaphoreType.DMA
    return pl.pallas_call(
        functools.partial(kernel, n, ncb, moved, cols * n),
        out_shape=jax.ShapeDtypeStruct((rows, cols), BF16),
        in_specs=[hbm, vm] + [hbm] * 4,
        out_specs=vm,
        scratch_shapes=[
            pltpu.VMEM((rows, cols), BF16),
            pltpu.VMEM((part, cols), BF16),
            pltpu.VMEM((part, cols), BF16),
            pltpu.VMEM((part, cols), BF16),
            pltpu.VMEM((2, cols, hidden), BF16),
            pltpu.VMEM((2, hidden, cols), BF16),
            pltpu.VMEM((most, part, cols), F32),
            pltpu.VMEM((rows, cols), BF16),
            pltpu.VMEM((1 + most, part, cols), BF16),
            pltpu.VMEM((2 * jobs, part, chunk), F32),
            pltpu.VMEM((2 * jobs, part, chunk), F32),
            pltpu.VMEM((part, cols), F32),
            pltpu.VMEM((part, 128), F32),
            pltpu.VMEM((2, 2 * jobs, PIECES, part, piece), BF16),
            pltpu.VMEM((2, 2 * jobs, PIECES, part, piece), BF16),
            pltpu.VMEM((3, most, 1, 128), F32),
            pltpu.VMEM((3, most, n, 1, 128), F32),
            pltpu.VMEM((2, most, part, cols), BF16),
            pltpu.VMEM((2, most, ncb, part, cols), BF16),
            dma,
            dma((4,)),
            dma((chunks,)),
            dma((3,)),
            dma((2,)),
            dma((2, jobs, PIECES)),
            dma,
            dma((3, most)),
            dma,
            dma((2, most)),
        ],
        compiler_params=pltpu.CompilerParams(
            collective_id=0, has_side_effects=True, vmem_limit_bytes=LIMIT * 1024
        ),
    )(
        tokens,
        jnp.stack([gain_first, gain_second, gain_last]),
        up_first,
        down_first,
        up_second,
        down_second,
    )


def solution(mesh):
    return jax.shard_map(
        functools.partial(local, mesh.shape["ra"], mesh.shape["cb"], mesh.shape["dp"]),
        mesh=mesh,
        in_specs=(
            P(("grp", "dp"), "ra"),
            P("ra"),
            P("ra", "cb"),
            P("cb", "ra"),
            P("ra"),
            P("ra", "cb"),
            P("cb", "ra"),
            P("ra"),
        ),
        out_specs=P(("grp", "dp"), "ra"),
        check_vma=False,
    )
```

```python
import functools

import jax
import jax.numpy as jnp
from jax import lax
from jax.experimental import pallas as pl
from jax.experimental.pallas import tpu as pltpu
from jax.sharding import PartitionSpec as P

EPS = 1e-06
MESH = pl.DeviceIdType.MESH
F32, BF16 = jnp.float32, jnp.bfloat16

CHUNK = 1024
SPLITS = 4
PIECES = 2
LAG10 = (40, 40)
SLACK = (2, 3)
LIMIT = 55100


def kernel(
    n,
    ncb,
    moved,
    width,
    tokens_ref,
    gains,
    up_first,
    down_first,
    up_second,
    down_second,
    out_ref,
    tokens_v,
    extra_v,
    done_v,
    back_v,
    up_v,
    down_v,
    h_v,
    entry_v,
    scaled_v,
    own_v,
    acc_v,
    branch_v,
    inv_v,
    send_v,
    recv_v,
    sq_send,
    sq_recv,
    cb_send,
    cb_recv,
    in_sem,
    pass_sem,
    up_sem,
    weight_sem,
    send_sem,
    recv_sem,
    sq_ssem,
    sq_rsem,
    cb_ssem,
    cb_rsem,
):
    k = lax.axis_index("ra")
    second = lax.axis_index("dp") > 0
    other_core = 1 - lax.axis_index("dp")
    cb = lax.axis_index("cb")
    hidden = up_v.shape[2]
    most, rows = h_v.shape[0], h_v.shape[1]
    chunk = own_v.shape[2]
    pieces = send_v.shape[2]
    piece = chunk // pieces
    chunks = hidden // chunk
    most_jobs = most * chunks
    swap = ncb == 2 and most - 2 * moved >= 2
    splits = jnp.where(second, most, most - 2 * moved)
    jobs = splits * chunks
    early = jnp.where(2 * k < n, 0, 1)
    late = 1 - early
    early_hops = jnp.where(early == 0, k, n - 1 - k)
    has_early = early_hops > 0
    early_to = jnp.where(early == 0, k + 1, k - 1)
    late_to = jnp.where(early_hops > 0, jnp.where(late == 0, k + 1, k - 1), early_to)
    lags = jnp.where(second, LAG10[1], LAG10[0])
    slack = jnp.where(second, SLACK[1], SLACK[0])
    depth = jnp.maximum(((n - 1 - 2 * early_hops) * lags + 9) // 10, 1)
    deepest = jnp.maximum(((n - 1) * lags + 9) // 10, 1)
    gap = jnp.maximum(chunks + deepest + slack - jobs, 0)
    if swap:
        gap = jnp.maximum(gap, deepest - (splits - 2) * chunks)
        gap = jnp.maximum(gap, deepest + slack - (splits - 1) * chunks)
    period = jobs + gap

    def up_copy(c):
        columns = pl.ds(c * chunk, chunk)
        return pltpu.make_async_copy(up_first.at[:, columns], up_v.at[0, :, columns], up_sem.at[c])

    def up_wait(c):
        columns = pl.ds(pl.multiple_of(c * chunk, chunk), chunk)
        pltpu.make_async_copy(
            up_first.at[:, columns], up_v.at[0, :, columns], up_sem.at[c]
        ).wait()

    up_next = pltpu.make_async_copy(up_second, up_v.at[1], weight_sem.at[2])

    def down_copy(layer):
        ref = (down_first, down_second)[layer]
        return pltpu.make_async_copy(ref, down_v.at[layer], weight_sem.at[layer])

    def split_of(level, slot):
        if not swap:
            return slot
        swapped = (lax.rem(cb + level, 2) == 0) & (slot >= splits - 2)
        return jnp.where(swapped, 2 * splits - 3 - slot, slot)

    tokens_in = pltpu.make_async_copy(tokens_ref, tokens_v, in_sem)
    tokens_in.start()
    up_copy(0).start()

    barrier = pltpu.get_barrier_semaphore()
    partners = [
        (i, j) for i in range(n) for j in range(ncb) if i + j > 0 and (swap or i * j == 0)
    ]
    for i, j in partners:
        pl.semaphore_signal(
            barrier,
            inc=1,
            device_id={"ra": lax.rem(k + i, n), "cb": lax.rem(cb + j, ncb)},
            device_id_type=MESH,
        )
    if moved:
        pl.semaphore_signal(
            barrier, inc=1, device_id={"dp": other_core}, device_id_type=MESH
        )

    def to_core(src, dst, i):
        return pltpu.make_async_remote_copy(
            src_ref=src,
            dst_ref=dst,
            send_sem=pass_sem.at[2 * i],
            recv_sem=pass_sem.at[2 * i + 1],
            device_id={"dp": other_core},
            device_id_type=MESH,
        )

    last = most - 1 - moved
    lent = to_core(tokens_v.at[pl.ds(last * rows, rows), :], extra_v, 0)
    given = to_core(done_v, back_v, 1)

    def tile_of(i):
        return i + jnp.where(second, moved, 0) if i > 1 else i

    tokens_in.wait()
    for c in range(1, chunks):
        up_copy(c).start()
    def multiply_first(c):
        up_wait(c)
        columns = pl.ds(pl.multiple_of(c * chunk, chunk), chunk)
        product = jnp.dot(entry_v[...], up_v[0, :, columns], preferred_element_type=F32)
        for i in range(most - moved):
            own_v[tile_of(i) * chunks + c] = product[i * rows : (i + 1) * rows, :]

    def multiply_extra():
        for c in range(chunks):
            columns = pl.ds(c * chunk, chunk)
            own_v[2 * chunks + c] = jnp.dot(
                scaled_v[0], up_v[0, :, columns], preferred_element_type=F32
            )

    ready = has_early
    for i in range(most - moved):
        tile = tokens_v[i * rows : (i + 1) * rows, :].astype(F32)
        h_v[tile_of(i)] = tile
        entry_v[i * rows : (i + 1) * rows, :] = (tile * gains[0:1, :]).astype(BF16)
    multiply_first(0)

    @pl.when(ready)
    def _():
        for c in range(1, chunks):
            multiply_first(c)

    pl.semaphore_wait(barrier, len(partners) + moved)
    if moved:

        @pl.when(jnp.logical_not(second))
        def _():
            lent.start()

    down_copy(0).start()
    up_next.start()
    down_copy(1).start()

    def chain(direction, job, p, to):
        return pltpu.make_async_remote_copy(
            src_ref=send_v.at[direction, job, p],
            dst_ref=recv_v.at[direction, job, p],
            send_sem=send_sem.at[direction],
            recv_sem=recv_sem.at[direction, lax.rem(job, most_jobs), p],
            device_id={"ra": to},
            device_id_type=MESH,
        )

    def sq_copy(level, t, to, to_cb):
        return pltpu.make_async_remote_copy(
            src_ref=sq_send.at[level, t],
            dst_ref=sq_recv.at[level, t, k],
            send_sem=sq_ssem,
            recv_sem=sq_rsem.at[level, t],
            device_id={"ra": to, "cb": to_cb},
            device_id_type=MESH,
        )

    def cb_copy(layer, t, to):
        return pltpu.make_async_remote_copy(
            src_ref=cb_send.at[layer, t],
            dst_ref=cb_recv.at[layer, t, cb],
            send_sem=cb_ssem,
            recv_sem=cb_rsem.at[layer, t],
            device_id={"cb": to},
            device_id_type=MESH,
        )

    def of_all(ref, ssem, rsem, axis, to):
        return pltpu.make_async_remote_copy(
            src_ref=ref,
            dst_ref=ref,
            send_sem=ssem,
            recv_sem=rsem,
            device_id={axis: to},
            device_id_type=MESH,
        )

    diagonal = lax.broadcasted_iota(jnp.int32, (rows, 128), 0) == lax.broadcasted_iota(
        jnp.int32, (rows, 128), 1
    )

    def send_squares(level, t, h32, across=False):
        total = jnp.sum(h32 * h32, axis=1, keepdims=True)
        line = jnp.sum(jnp.where(diagonal, total, 0.0), axis=0, keepdims=True)
        sq_send[level, t] = line
        sq_recv[level, t, k] = line
        for off in range(1, n):
            sq_copy(level, t, lax.rem(k + off, n), cb).start()
        if across:
            for off in range(n):
                sq_copy(level, t, lax.rem(k + off, n), lax.rem(cb + 1, ncb)).start()

    def wait_squares(level, t, count):
        peers = sq_recv.at[level, t, pl.ds(0, count)]
        of_all(peers, sq_ssem, sq_rsem.at[level, t], "ra", lax.rem(k + 1, n)).wait_recv()

    def inverse_of(level, t):
        total = sq_recv[level, t, 0]
        for source in range(1, n):
            total = total + sq_recv[level, t, source]
        line = lax.rsqrt(total * (1.0 / width) + EPS)
        column = jnp.sum(jnp.where(diagonal, line, 0.0), axis=1, keepdims=True)
        return jnp.broadcast_to(column, (rows, 128))

    def gather_branch(layer, t):
        peers = cb_recv.at[layer, t, pl.ds(0, ncb - 1)]
        of_all(peers, cb_ssem, cb_rsem.at[layer, t], "cb", lax.rem(cb + 1, ncb)).wait_recv()
        total = cb_recv[layer, t, 0].astype(F32)
        for source in range(1, ncb):
            total = total + cb_recv[layer, t, source].astype(F32)
        return (0.5 * h_v[t] + total).astype(BF16).astype(F32)

    def multiply_up(t, c):
        columns = pl.ds(pl.multiple_of(c * chunk, chunk), chunk)
        own_v[(most + t) * chunks + c] = jnp.dot(
            scaled_v[1 + t], up_v[1, :, columns], preferred_element_type=F32
        )

    def multiply_down(level, job, c):
        total = None
        for p in range(pieces):
            at = slice(p * piece, (p + 1) * piece)
            pre = (recv_v[late, job, p].astype(F32) + acc_v[job, :, at]) * inv_v[:, 0:1]
            act = jnp.square(jnp.maximum(pre, 0.0)).astype(BF16)
            rows_at = pl.ds(pl.multiple_of(c * chunk + p * piece, piece), piece)
            part = jnp.dot(act, down_v[level, rows_at, :], preferred_element_type=F32)
            total = part if total is None else total + part
        branch_v[...] = jnp.where(c == 0, 0.0, branch_v[...]) + total

    branch_v[...] = jnp.zeros_like(branch_v)

    def place(s):
        level = jnp.where(s < period, 0, jnp.where(s < 2 * period, 1, 2))
        at = s - level * period
        live = at < jobs
        slot = jnp.where(live, at // chunks, 0)
        return level, at, live, slot, at % chunks

    steps = 2 * jobs + gap + deepest
    plain = splits - 2 if swap else splits

    def close(j):
        h32 = gather_branch(1, j)
        h_v[j] = h32
        send_squares(2, j, h32)

    def first_squares():
        for i in range(most):

            @pl.when((i < splits) & jnp.logical_not(second & (i == 2 * moved) & (moved > 0)))
            def _():
                send_squares(0, i, h_v[i])

    @pl.when(has_early)
    def _():
        first_squares()

    def step(s, _):
        s2 = s - depth
        level2 = jnp.where(s2 < period, 0, 1)
        at2 = s2 - level2 * period
        live2 = (s2 >= 0) & (at2 < jobs)
        at2 = jnp.where(live2, at2, 0)
        t2 = split_of(level2, at2 // chunks)
        c2 = at2 % chunks
        job2 = level2 * most_jobs + at2

        level, at, live, slot, c = place(s)
        t = split_of(level, slot)
        job = level * most_jobs + at
        own_at = (level * most + t) * chunks + c
        sending = live & (level < 2)

        own_at2 = (level2 * most + t2) * chunks + c2
        for p in range(pieces):
            part = slice(p * piece, (p + 1) * piece)

            @pl.when(live2)
            def _():
                chain(late, job2, p, late_to).wait_recv()

                @pl.when(has_early)
                def _():
                    total = recv_v[late, job2, p].astype(F32) + own_v[own_at2, :, part]
                    send_v[late, job2, p] = total.astype(BF16)
                    chain(late, job2, p, late_to).start()

            @pl.when(sending)
            def _():
                own = own_v[own_at, :, part]

                @pl.when(has_early)
                def _():
                    chain(early, job, p, early_to).wait_recv()
                    total = recv_v[early, job, p].astype(F32) + own
                    send_v[early, job, p] = total.astype(BF16)
                    acc_v[job, :, part] = total

                @pl.when(jnp.logical_not(has_early))
                def _():
                    send_v[early, job, p] = own.astype(BF16)
                    acc_v[job, :, part] = own

                chain(early, job, p, early_to).start()

        @pl.when((s == 0) & jnp.logical_not(has_early))
        def _():
            first_squares()

        if moved:

            @pl.when(second & (s == chunks - 1))
            def _():
                lent.wait_recv()
                h32 = extra_v[...].astype(F32)
                h_v[2] = h32
                scaled_v[0] = (h32 * gains[0:1, :]).astype(BF16)
                multiply_extra()
                send_squares(0, 2, h32)

        @pl.when(sending & (level == 1) & (c == 0) & jnp.logical_not(has_early))
        def _():
            send_squares(1, t, h_v[t])

        @pl.when(live2 & (c2 == 0))
        def _():
            wait_squares(level2, t2, n - 1)
            inv_v[...] = inverse_of(level2, t2)

        for layer in range(2):

            @pl.when(live2 & (job2 == layer * most_jobs))
            def _():
                down_copy(layer).wait()

        level3, at3, live3, slot3, c3 = place(s + 1)
        t3 = split_of(level3, slot3)
        ahead = live3 & (level3 == 1)
        both = live2 & ahead & (c3 > 0)

        @pl.when(both)
        def _():
            multiply_up(t3, c3)
            multiply_down(level2, job2, c2)

        @pl.when(live2 & jnp.logical_not(both))
        def _():
            multiply_down(level2, job2, c2)

        @pl.when(live2 & (c2 == chunks - 1))
        def _():
            value = branch_v[...].astype(BF16)
            cb_send[level2, t2] = value
            cb_recv[level2, t2, cb] = value
            for off in range(1, ncb):
                cb_copy(level2, t2, lax.rem(cb + off, ncb)).start()

        @pl.when(ahead & (c3 == 0))
        def _():
            h32 = gather_branch(0, t3)
            h_v[t3] = h32
            scaled_v[1 + t3] = (h32 * gains[1:1 + 1, :]).astype(BF16)

            @pl.when(at3 == 0)
            def _():
                up_next.wait()

        @pl.when(ahead & jnp.logical_not(both))
        def _():
            multiply_up(t3, c3)

        @pl.when(ahead & (c3 == 0) & has_early)
        def _():
            send_squares(1, t3, h_v[t3])

        @pl.when(live3 & (level3 == 0) & (at3 < chunks) & jnp.logical_not(ready))
        def _():
            multiply_first(c3)

        for j in range(most):

            @pl.when((j < plain) & (s == 2 * period + j * chunks))
            def _():
                close(j)

        return 0

    lax.fori_loop(0, steps, step, 0)

    def normed(t):
        inv = inverse_of(2, t)[:, 0:1]
        return (h_v[t] * inv * gains[2:3, :]).astype(BF16)

    def finish(t):
        row = t - jnp.where(second & (t > 2), moved, 0)
        out_ref[pl.ds(pl.multiple_of(row * rows, rows), rows), :] = normed(t)

    if swap:
        mine = split_of(1, splits - 1)
        other = split_of(1, splits - 2)
        h32 = gather_branch(1, mine)
        h_v[mine] = h32
        send_squares(2, mine, h32, across=True)
    for j in range(most):

        @pl.when((j < plain) & (2 * period + j * chunks >= steps))
        def _():
            close(j)

    order = [2, 0, 1] + list(range(3, most)) if moved else list(range(most))
    for j in order:

        @pl.when(j < plain)
        def _():
            wait_squares(2, j, n - 1)
            if moved and j == 2:

                @pl.when(second)
                def _():
                    done_v[...] = normed(2)
                    given.start()

                @pl.when(jnp.logical_not(second))
                def _():
                    finish(2)

            else:
                finish(j)

    if swap:
        h_v[other] = gather_branch(1, other)
        wait_squares(2, other, n)
        finish(other)
        wait_squares(2, mine, n - 1)
        finish(mine)

    def wait_sends(count):
        sent = 2 * count * chunks
        of_all(
            send_v.at[early, pl.ds(0, sent)],
            send_sem.at[early],
            recv_sem.at[early, 0, 0],
            "ra",
            early_to,
        ).wait_send()

        @pl.when(has_early)
        def _():
            of_all(
                send_v.at[late, pl.ds(0, sent)],
                send_sem.at[late],
                recv_sem.at[late, 0, 0],
                "ra",
                late_to,
            ).wait_send()

        peers = sq_recv.at[:, pl.ds(0, count), pl.ds(0, n - 1)]
        of_all(peers, sq_ssem, sq_rsem.at[0, 0], "ra", lax.rem(k + 1, n)).wait_send()
        if swap:
            one = sq_recv.at[0, 0, pl.ds(0, 1)]
            of_all(one, sq_ssem, sq_rsem.at[0, 0], "ra", lax.rem(k + 1, n)).wait_send()
        peers = cb_recv.at[:, pl.ds(0, count), pl.ds(0, ncb - 1)]
        of_all(peers, cb_ssem, cb_rsem.at[0, 0], "cb", lax.rem(cb + 1, ncb)).wait_send()

    if moved:

        @pl.when(second)
        def _():
            wait_sends(most)
            given.wait_send()

        @pl.when(jnp.logical_not(second))
        def _():
            wait_sends(most - 2)
            lent.wait_send()
            given.wait_recv()
            out_ref[last * rows : (last + 1) * rows, :] = back_v[...]

    else:
        wait_sends(most)


def local(n, ncb, ndp, *args):
    tokens, gain_first, up_first, down_first, gain_second, up_second, down_second, gain_last = args
    rows, cols = tokens.shape
    hidden = up_first.shape[1]
    chunk = min(CHUNK, hidden)
    chunks = hidden // chunk
    splits = SPLITS if rows % (16 * SPLITS) == 0 else 1
    part = rows // splits
    moved = int(ndp == 2 and splits >= 4)
    most = splits + moved
    jobs = most * chunks
    piece = chunk // PIECES
    hbm = pl.BlockSpec(memory_space=pl.ANY)
    vm = pl.BlockSpec(memory_space=pltpu.VMEM)
    dma = pltpu.SemaphoreType.DMA
    return pl.pallas_call(
        functools.partial(kernel, n, ncb, moved, cols * n),
        out_shape=jax.ShapeDtypeStruct((rows, cols), BF16),
        in_specs=[hbm, vm] + [hbm] * 4,
        out_specs=vm,
        scratch_shapes=[
            pltpu.VMEM((rows, cols), BF16),
            pltpu.VMEM((part, cols), BF16),
            pltpu.VMEM((part, cols), BF16),
            pltpu.VMEM((part, cols), BF16),
            pltpu.VMEM((2, cols, hidden), BF16),
            pltpu.VMEM((2, hidden, cols), BF16),
            pltpu.VMEM((most, part, cols), F32),
            pltpu.VMEM((rows, cols), BF16),
            pltpu.VMEM((1 + most, part, cols), BF16),
            pltpu.VMEM((2 * jobs, part, chunk), F32),
            pltpu.VMEM((2 * jobs, part, chunk), F32),
            pltpu.VMEM((part, cols), F32),
            pltpu.VMEM((part, 128), F32),
            pltpu.VMEM((2, 2 * jobs, PIECES, part, piece), BF16),
            pltpu.VMEM((2, 2 * jobs, PIECES, part, piece), BF16),
            pltpu.VMEM((3, most, 1, 128), F32),
            pltpu.VMEM((3, most, n, 1, 128), F32),
            pltpu.VMEM((2, most, part, cols), BF16),
            pltpu.VMEM((2, most, ncb, part, cols), BF16),
            dma,
            dma((4,)),
            dma((chunks,)),
            dma((3,)),
            dma((2,)),
            dma((2, jobs, PIECES)),
            dma,
            dma((3, most)),
            dma,
            dma((2, most)),
        ],
        compiler_params=pltpu.CompilerParams(
            collective_id=0, has_side_effects=True, vmem_limit_bytes=LIMIT * 1024
        ),
    )(
        tokens,
        jnp.stack([gain_first, gain_second, gain_last]),
        up_first,
        down_first,
        up_second,
        down_second,
    )


def solution(mesh):
    return jax.shard_map(
        functools.partial(local, mesh.shape["ra"], mesh.shape["cb"], mesh.shape["dp"]),
        mesh=mesh,
        in_specs=(
            P(("grp", "dp"), "ra"),
            P("ra"),
            P("ra", "cb"),
            P("cb", "ra"),
            P("ra"),
            P("ra", "cb"),
            P("cb", "ra"),
            P("ra"),
        ),
        out_specs=P(("grp", "dp"), "ra"),
        check_vma=False,
    )
```

```python
import functools

import jax
import jax.numpy as jnp
from jax import lax
from jax.experimental import pallas as pl
from jax.experimental.pallas import tpu as pltpu
from jax.sharding import PartitionSpec as P

EPS = 1e-06
MESH = pl.DeviceIdType.MESH
F32, BF16 = jnp.float32, jnp.bfloat16

CHUNK = 1024
SPLITS = 4
PIECES = 2
RING = 16
LAG10 = (40, 40)
SLACK = (2, 3)
LIMIT = 55100


def kernel(
    n,
    ncb,
    moved,
    width,
    tokens_ref,
    gains,
    up_first,
    down_first,
    up_second,
    down_second,
    out_ref,
    tokens_v,
    extra_v,
    done_v,
    back_v,
    up_v,
    down_v,
    h_v,
    entry_v,
    scaled_v,
    own_v,
    acc_v,
    branch_v,
    inv_v,
    send_v,
    recv_v,
    sq_send,
    sq_recv,
    cb_send,
    cb_recv,
    in_sem,
    pass_sem,
    up_sem,
    weight_sem,
    send_sem,
    recv_sem,
    sq_ssem,
    sq_rsem,
    cb_ssem,
    cb_rsem,
):
    k = lax.axis_index("ra")
    second = lax.axis_index("dp") > 0
    other_core = 1 - lax.axis_index("dp")
    cb = lax.axis_index("cb")
    hidden = up_v.shape[2]
    most, rows = h_v.shape[0], h_v.shape[1]
    chunk = own_v.shape[2]
    pieces = send_v.shape[2]
    piece = chunk // pieces
    chunks = hidden // chunk
    most_jobs = most * chunks
    swap = ncb == 2 and most - 2 * moved >= 2
    splits = jnp.where(second, most, most - 2 * moved)
    jobs = splits * chunks
    early = jnp.where(2 * k < n, 0, 1)
    late = 1 - early
    early_hops = jnp.where(early == 0, k, n - 1 - k)
    has_early = early_hops > 0
    early_to = jnp.where(early == 0, k + 1, k - 1)
    late_to = jnp.where(early_hops > 0, jnp.where(late == 0, k + 1, k - 1), early_to)
    lags = jnp.where(second, LAG10[1], LAG10[0])
    slack = jnp.where(second, SLACK[1], SLACK[0])
    depth = jnp.maximum(((n - 1 - 2 * early_hops) * lags + 9) // 10, 1)
    deepest = jnp.maximum(((n - 1) * lags + 9) // 10, 1)
    gap = jnp.maximum(chunks + deepest + slack - jobs, 0)
    if swap:
        gap = jnp.maximum(gap, deepest - (splits - 2) * chunks)
        gap = jnp.maximum(gap, deepest + slack - (splits - 1) * chunks)
    period = jobs + gap

    def up_copy(c):
        columns = pl.ds(c * chunk, chunk)
        return pltpu.make_async_copy(up_first.at[:, columns], up_v.at[0, :, columns], up_sem.at[c])

    def up_wait(c):
        columns = pl.ds(pl.multiple_of(c * chunk, chunk), chunk)
        pltpu.make_async_copy(
            up_first.at[:, columns], up_v.at[0, :, columns], up_sem.at[c]
        ).wait()

    up_next = pltpu.make_async_copy(up_second, up_v.at[1], weight_sem.at[2])

    def down_copy(layer):
        ref = (down_first, down_second)[layer]
        return pltpu.make_async_copy(ref, down_v.at[layer], weight_sem.at[layer])

    def split_of(level, slot):
        if not swap:
            return slot
        swapped = (lax.rem(cb + level, 2) == 0) & (slot >= splits - 2)
        return jnp.where(swapped, 2 * splits - 3 - slot, slot)

    tokens_in = pltpu.make_async_copy(tokens_ref, tokens_v, in_sem)
    tokens_in.start()
    up_copy(0).start()

    barrier = pltpu.get_barrier_semaphore()
    partners = [
        (i, j) for i in range(n) for j in range(ncb) if i + j > 0 and (swap or i * j == 0)
    ]
    for i, j in partners:
        pl.semaphore_signal(
            barrier,
            inc=1,
            device_id={"ra": lax.rem(k + i, n), "cb": lax.rem(cb + j, ncb)},
            device_id_type=MESH,
        )
    if moved:
        pl.semaphore_signal(
            barrier, inc=1, device_id={"dp": other_core}, device_id_type=MESH
        )

    def to_core(src, dst, i):
        return pltpu.make_async_remote_copy(
            src_ref=src,
            dst_ref=dst,
            send_sem=pass_sem.at[2 * i],
            recv_sem=pass_sem.at[2 * i + 1],
            device_id={"dp": other_core},
            device_id_type=MESH,
        )

    last = most - 1 - moved
    lent = to_core(tokens_v.at[pl.ds(last * rows, rows), :], extra_v, 0)
    given = to_core(done_v, back_v, 1)

    def tile_of(i):
        return i + jnp.where(second, moved, 0) if i > 1 else i

    tokens_in.wait()
    for c in range(1, chunks):
        up_copy(c).start()
    def multiply_first(c):
        up_wait(c)
        columns = pl.ds(pl.multiple_of(c * chunk, chunk), chunk)
        product = jnp.dot(entry_v[...], up_v[0, :, columns], preferred_element_type=F32)
        for i in range(most - moved):
            own_v[tile_of(i) * chunks + c] = product[i * rows : (i + 1) * rows, :]

    def multiply_extra():
        for c in range(chunks):
            columns = pl.ds(c * chunk, chunk)
            own_v[2 * chunks + c] = jnp.dot(
                scaled_v[0], up_v[0, :, columns], preferred_element_type=F32
            )

    ready = has_early
    for i in range(most - moved):
        tile = tokens_v[i * rows : (i + 1) * rows, :].astype(F32)
        h_v[tile_of(i)] = tile
        entry_v[i * rows : (i + 1) * rows, :] = (tile * gains[0:1, :]).astype(BF16)
    multiply_first(0)

    @pl.when(ready)
    def _():
        for c in range(1, chunks):
            multiply_first(c)

    pl.semaphore_wait(barrier, len(partners) + moved)
    if moved:

        @pl.when(jnp.logical_not(second))
        def _():
            lent.start()

    down_copy(0).start()
    up_next.start()
    down_copy(1).start()

    def chain(direction, job, p, to):
        return pltpu.make_async_remote_copy(
            src_ref=send_v.at[direction, job, p],
            dst_ref=recv_v.at[direction, job, p],
            send_sem=send_sem.at[direction],
            recv_sem=recv_sem.at[direction, lax.rem(job, recv_sem.shape[1]), p],
            device_id={"ra": to},
            device_id_type=MESH,
        )

    def sq_copy(level, t, to, to_cb):
        return pltpu.make_async_remote_copy(
            src_ref=sq_send.at[level, t],
            dst_ref=sq_recv.at[level, t, k],
            send_sem=sq_ssem,
            recv_sem=sq_rsem.at[level, t],
            device_id={"ra": to, "cb": to_cb},
            device_id_type=MESH,
        )

    def cb_copy(layer, t, to):
        return pltpu.make_async_remote_copy(
            src_ref=cb_send.at[layer, t],
            dst_ref=cb_recv.at[layer, t, cb],
            send_sem=cb_ssem,
            recv_sem=cb_rsem.at[layer, t],
            device_id={"cb": to},
            device_id_type=MESH,
        )

    def of_all(ref, ssem, rsem, axis, to):
        return pltpu.make_async_remote_copy(
            src_ref=ref,
            dst_ref=ref,
            send_sem=ssem,
            recv_sem=rsem,
            device_id={axis: to},
            device_id_type=MESH,
        )

    diagonal = lax.broadcasted_iota(jnp.int32, (rows, 128), 0) == lax.broadcasted_iota(
        jnp.int32, (rows, 128), 1
    )

    def send_squares(level, t, h32, across=False):
        total = jnp.sum(h32 * h32, axis=1, keepdims=True)
        line = jnp.sum(jnp.where(diagonal, total, 0.0), axis=0, keepdims=True)
        sq_send[level, t] = line
        sq_recv[level, t, k] = line
        for off in range(1, n):
            sq_copy(level, t, lax.rem(k + off, n), cb).start()
        if across:
            for off in range(n):
                sq_copy(level, t, lax.rem(k + off, n), lax.rem(cb + 1, ncb)).start()

    def wait_squares(level, t, count):
        peers = sq_recv.at[level, t, pl.ds(0, count)]
        of_all(peers, sq_ssem, sq_rsem.at[level, t], "ra", lax.rem(k + 1, n)).wait_recv()

    def inverse_of(level, t):
        total = sq_recv[level, t, 0]
        for source in range(1, n):
            total = total + sq_recv[level, t, source]
        line = lax.rsqrt(total * (1.0 / width) + EPS)
        column = jnp.sum(jnp.where(diagonal, line, 0.0), axis=1, keepdims=True)
        return jnp.broadcast_to(column, (rows, 128))

    def gather_branch(layer, t):
        peers = cb_recv.at[layer, t, pl.ds(0, ncb - 1)]
        of_all(peers, cb_ssem, cb_rsem.at[layer, t], "cb", lax.rem(cb + 1, ncb)).wait_recv()
        total = cb_recv[layer, t, 0].astype(F32)
        for source in range(1, ncb):
            total = total + cb_recv[layer, t, source].astype(F32)
        return (0.5 * h_v[t] + total).astype(BF16).astype(F32)

    def multiply_up(t, c):
        columns = pl.ds(pl.multiple_of(c * chunk, chunk), chunk)
        own_v[(most + t) * chunks + c] = jnp.dot(
            scaled_v[1 + t], up_v[1, :, columns], preferred_element_type=F32
        )

    def multiply_down(level, job, c):
        total = None
        for p in range(pieces):
            at = slice(p * piece, (p + 1) * piece)
            pre = (recv_v[late, job, p].astype(F32) + acc_v[job, :, at]) * inv_v[:, 0:1]
            act = jnp.square(jnp.maximum(pre, 0.0)).astype(BF16)
            rows_at = pl.ds(pl.multiple_of(c * chunk + p * piece, piece), piece)
            part = jnp.dot(act, down_v[level, rows_at, :], preferred_element_type=F32)
            total = part if total is None else total + part
        branch_v[...] = jnp.where(c == 0, 0.0, branch_v[...]) + total

    branch_v[...] = jnp.zeros_like(branch_v)

    def place(s):
        level = jnp.where(s < period, 0, jnp.where(s < 2 * period, 1, 2))
        at = s - level * period
        live = at < jobs
        slot = jnp.where(live, at // chunks, 0)
        return level, at, live, slot, at % chunks

    steps = 2 * jobs + gap + deepest
    plain = splits - 2 if swap else splits

    def close(j):
        h32 = gather_branch(1, j)
        h_v[j] = h32
        send_squares(2, j, h32)

    def first_squares():
        for i in range(most):

            @pl.when((i < splits) & jnp.logical_not(second & (i == 2 * moved) & (moved > 0)))
            def _():
                send_squares(0, i, h_v[i])

    @pl.when(has_early)
    def _():
        first_squares()

    def step(s, _):
        s2 = s - depth
        level2 = jnp.where(s2 < period, 0, 1)
        at2 = s2 - level2 * period
        live2 = (s2 >= 0) & (at2 < jobs)
        at2 = jnp.where(live2, at2, 0)
        t2 = split_of(level2, at2 // chunks)
        c2 = at2 % chunks
        job2 = level2 * most_jobs + at2

        level, at, live, slot, c = place(s)
        t = split_of(level, slot)
        job = level * most_jobs + at
        own_at = (level * most + t) * chunks + c
        sending = live & (level < 2)

        own_at2 = (level2 * most + t2) * chunks + c2
        for p in range(pieces):
            part = slice(p * piece, (p + 1) * piece)

            @pl.when(live2)
            def _():
                chain(late, job2, p, late_to).wait_recv()

                @pl.when(has_early)
                def _():
                    total = recv_v[late, job2, p].astype(F32) + own_v[own_at2, :, part]
                    send_v[late, job2, p] = total.astype(BF16)
                    chain(late, job2, p, late_to).start()

            @pl.when(sending)
            def _():
                own = own_v[own_at, :, part]

                @pl.when(has_early)
                def _():
                    chain(early, job, p, early_to).wait_recv()
                    total = recv_v[early, job, p].astype(F32) + own
                    send_v[early, job, p] = total.astype(BF16)
                    acc_v[job, :, part] = total

                @pl.when(jnp.logical_not(has_early))
                def _():
                    send_v[early, job, p] = own.astype(BF16)
                    acc_v[job, :, part] = own

                chain(early, job, p, early_to).start()

        @pl.when((s == 0) & jnp.logical_not(has_early))
        def _():
            first_squares()

        if moved:

            @pl.when(second & (s == chunks - 1))
            def _():
                lent.wait_recv()
                h32 = extra_v[...].astype(F32)
                h_v[2] = h32
                scaled_v[0] = (h32 * gains[0:1, :]).astype(BF16)
                multiply_extra()
                send_squares(0, 2, h32)

        @pl.when(sending & (level == 1) & (c == 0) & jnp.logical_not(has_early))
        def _():
            send_squares(1, t, h_v[t])

        @pl.when(live2 & (c2 == 0))
        def _():
            wait_squares(level2, t2, n - 1)
            inv_v[...] = inverse_of(level2, t2)

        for layer in range(2):

            @pl.when(live2 & (job2 == layer * most_jobs))
            def _():
                down_copy(layer).wait()

        level3, at3, live3, slot3, c3 = place(s + 1)
        t3 = split_of(level3, slot3)
        ahead = live3 & (level3 == 1)
        both = live2 & ahead & (c3 > 0)

        @pl.when(both)
        def _():
            multiply_up(t3, c3)
            multiply_down(level2, job2, c2)

        @pl.when(live2 & jnp.logical_not(both))
        def _():
            multiply_down(level2, job2, c2)

        @pl.when(live2 & (c2 == chunks - 1))
        def _():
            value = branch_v[...].astype(BF16)
            cb_send[level2, t2] = value
            cb_recv[level2, t2, cb] = value
            for off in range(1, ncb):
                cb_copy(level2, t2, lax.rem(cb + off, ncb)).start()

        @pl.when(ahead & (c3 == 0))
        def _():
            h32 = gather_branch(0, t3)
            h_v[t3] = h32
            scaled_v[1 + t3] = (h32 * gains[1:1 + 1, :]).astype(BF16)

            @pl.when(at3 == 0)
            def _():
                up_next.wait()

        @pl.when(ahead & jnp.logical_not(both))
        def _():
            multiply_up(t3, c3)

        @pl.when(ahead & (c3 == 0) & has_early)
        def _():
            send_squares(1, t3, h_v[t3])

        @pl.when(live3 & (level3 == 0) & (at3 < chunks) & jnp.logical_not(ready))
        def _():
            multiply_first(c3)

        for j in range(most):

            @pl.when((j < plain) & (s == 2 * period + j * chunks))
            def _():
                close(j)

        return 0

    lax.fori_loop(0, steps, step, 0)

    def normed(t):
        inv = inverse_of(2, t)[:, 0:1]
        return (h_v[t] * inv * gains[2:3, :]).astype(BF16)

    def finish(t):
        row = t - jnp.where(second & (t > 2), moved, 0)
        out_ref[pl.ds(pl.multiple_of(row * rows, rows), rows), :] = normed(t)

    if swap:
        mine = split_of(1, splits - 1)
        other = split_of(1, splits - 2)
        h32 = gather_branch(1, mine)
        h_v[mine] = h32
        send_squares(2, mine, h32, across=True)
    for j in range(most):

        @pl.when((j < plain) & (2 * period + j * chunks >= steps))
        def _():
            close(j)

    order = [2, 0, 1] + list(range(3, most)) if moved else list(range(most))
    for j in order:

        @pl.when(j < plain)
        def _():
            wait_squares(2, j, n - 1)
            if moved and j == 2:

                @pl.when(second)
                def _():
                    done_v[...] = normed(2)
                    given.start()

                @pl.when(jnp.logical_not(second))
                def _():
                    finish(2)

            else:
                finish(j)

    if swap:
        h_v[other] = gather_branch(1, other)
        wait_squares(2, other, n)
        finish(other)
        wait_squares(2, mine, n - 1)
        finish(mine)

    def wait_sends(count):
        sent = 2 * count * chunks
        of_all(
            send_v.at[early, pl.ds(0, sent)],
            send_sem.at[early],
            recv_sem.at[early, 0, 0],
            "ra",
            early_to,
        ).wait_send()

        @pl.when(has_early)
        def _():
            of_all(
                send_v.at[late, pl.ds(0, sent)],
                send_sem.at[late],
                recv_sem.at[late, 0, 0],
                "ra",
                late_to,
            ).wait_send()

        peers = sq_recv.at[:, pl.ds(0, count), pl.ds(0, n - 1)]
        of_all(peers, sq_ssem, sq_rsem.at[0, 0], "ra", lax.rem(k + 1, n)).wait_send()
        if swap:
            one = sq_recv.at[0, 0, pl.ds(0, 1)]
            of_all(one, sq_ssem, sq_rsem.at[0, 0], "ra", lax.rem(k + 1, n)).wait_send()
        peers = cb_recv.at[:, pl.ds(0, count), pl.ds(0, ncb - 1)]
        of_all(peers, cb_ssem, cb_rsem.at[0, 0], "cb", lax.rem(cb + 1, ncb)).wait_send()

    if moved:

        @pl.when(second)
        def _():
            wait_sends(most)
            given.wait_send()

        @pl.when(jnp.logical_not(second))
        def _():
            wait_sends(most - 2)
            lent.wait_send()
            given.wait_recv()
            out_ref[last * rows : (last + 1) * rows, :] = back_v[...]

    else:
        wait_sends(most)


def local(n, ncb, ndp, *args):
    tokens, gain_first, up_first, down_first, gain_second, up_second, down_second, gain_last = args
    rows, cols = tokens.shape
    hidden = up_first.shape[1]
    chunk = min(CHUNK, hidden)
    chunks = hidden // chunk
    splits = SPLITS if rows % (16 * SPLITS) == 0 else 1
    part = rows // splits
    moved = int(ndp == 2 and splits >= 4)
    most = splits + moved
    jobs = most * chunks
    piece = chunk // PIECES
    hbm = pl.BlockSpec(memory_space=pl.ANY)
    vm = pl.BlockSpec(memory_space=pltpu.VMEM)
    dma = pltpu.SemaphoreType.DMA
    return pl.pallas_call(
        functools.partial(kernel, n, ncb, moved, cols * n),
        out_shape=jax.ShapeDtypeStruct((rows, cols), BF16),
        in_specs=[hbm, vm] + [hbm] * 4,
        out_specs=vm,
        scratch_shapes=[
            pltpu.VMEM((rows, cols), BF16),
            pltpu.VMEM((part, cols), BF16),
            pltpu.VMEM((part, cols), BF16),
            pltpu.VMEM((part, cols), BF16),
            pltpu.VMEM((2, cols, hidden), BF16),
            pltpu.VMEM((2, hidden, cols), BF16),
            pltpu.VMEM((most, part, cols), F32),
            pltpu.VMEM((rows, cols), BF16),
            pltpu.VMEM((1 + most, part, cols), BF16),
            pltpu.VMEM((2 * jobs, part, chunk), F32),
            pltpu.VMEM((2 * jobs, part, chunk), F32),
            pltpu.VMEM((part, cols), F32),
            pltpu.VMEM((part, 128), F32),
            pltpu.VMEM((2, 2 * jobs, PIECES, part, piece), BF16),
            pltpu.VMEM((2, 2 * jobs, PIECES, part, piece), BF16),
            pltpu.VMEM((3, most, 1, 128), F32),
            pltpu.VMEM((3, most, n, 1, 128), F32),
            pltpu.VMEM((2, most, part, cols), BF16),
            pltpu.VMEM((2, most, ncb, part, cols), BF16),
            dma,
            dma((4,)),
            dma((chunks,)),
            dma((3,)),
            dma((2,)),
            dma((2, min(jobs, RING) if n == 4 else jobs, PIECES)),
            dma,
            dma((3, most)),
            dma,
            dma((2, most)),
        ],
        compiler_params=pltpu.CompilerParams(
            collective_id=0, has_side_effects=True, vmem_limit_bytes=LIMIT * 1024
        ),
    )(
        tokens,
        jnp.stack([gain_first, gain_second, gain_last]),
        up_first,
        down_first,
        up_second,
        down_second,
    )


def solution(mesh):
    return jax.shard_map(
        functools.partial(local, mesh.shape["ra"], mesh.shape["cb"], mesh.shape["dp"]),
        mesh=mesh,
        in_specs=(
            P(("grp", "dp"), "ra"),
            P("ra"),
            P("ra", "cb"),
            P("cb", "ra"),
            P("ra"),
            P("ra", "cb"),
            P("cb", "ra"),
            P("ra"),
        ),
        out_specs=P(("grp", "dp"), "ra"),
        check_vma=False,
    )
```
